32 devices in a mesh: sp: 8 (over z, y), tp: 4 (over x, core).
Axes of the slice: x: 2, y: 2, z: 4, core: 2. Of those that a mesh axis runs over, the one named last changes fastest.
Arguments:
- tokens: bfloat16 [4, 2048, 1024], P(None, ('sp', 'tp')), may hold values from -6 to 6
- norm_gain: float32 [1024], replicated, may hold values from 0.1 to 1.9
- x_weight: bfloat16 [1024, 1024], P('sp', 'tp'), may hold values from -0.1875 to 0.1875
- z_weight: bfloat16 [1024, 1024], P('sp', 'tp'), may hold values from -0.1875 to 0.1875
- b_weight: bfloat16 [1024, 1024], P('sp', 'tp'), may hold values from -0.1875 to 0.1875
- c_weight: bfloat16 [1024, 1024], P('sp', 'tp'), may hold values from -0.1875 to 0.1875
- dt_weight: bfloat16 [1024, 16], P('sp', 'tp'), may hold values from -0.1875 to 0.1875
- x_conv: float32 [4, 1024], P(None, 'tp'), may hold values from -3 to 3
- b_conv: float32 [4, 1024], P(None, 'tp'), may hold values from -3 to 3
- c_conv: float32 [4, 1024], P(None, 'tp'), may hold values from -3 to 3
- dt_bias: float32 [16], P('tp'), may hold values from -1 to 1
- decay_rate: float32 [16], P('tp'), may hold values from 0.15 to 3.5
- out_gain: float32 [1024], P('tp'), may hold values from 0.1 to 1.9
- out_weight: bfloat16 [1024, 1024], P('tp', 'sp'), may hold values from -0.1875 to 0.1875
Outputs:
- mixed: bfloat16 [4, 2048, 1024], P(None, ('sp', 'tp'))
The draws below stay inside these ranges and needn't reach their ends.
All inputs are finite; a program needn't handle non-finite values.
Results may differ from the reference program's by a relative error of at most 0.02.
Values may be sent and summed in bfloat16 or wider, within the bound.
A program may use at most 64 MiB of HBM per device.

```python
import math
import jax
import jax.numpy as jnp
from jax import lax

D = 1024
HEADS = 16
HEAD_P = 64
STATE = 128
GROUPS = 8
CONV = 4
BLOCK = 32
SEQS = 4
INNER = 1024
LENGTH = 2048


def shard_levels(own_key, shape, split, low, largest):
    def one(dim, shards_of):
        heights = jax.random.uniform(jax.random.fold_in(jax.random.fold_in(own_key, 6), dim), (shards_of,), jnp.float32, low / len(split), largest / len(split))
        return jnp.repeat(jnp.exp(heights), shape[dim] // shards_of).reshape((-1,) + (1,) * (len(shape) - dim - 1))

    gain = one(*split[0])
    for cut in split[1:]:
        gain = gain * one(*cut)
    return gain


def centred(rng, dims, deviation, most, split=(), kind=jnp.bfloat16):
    array = jax.random.normal(rng, dims, jnp.float32) * deviation
    if len(split) > 0:
        array = shard_levels(rng, dims, split, -0.22, 0.18) * array
    return jnp.clip(array, min=-most, max=most).astype(kind)


def setup_inputs(seed: int = 0) -> dict:
    arg_keys = jax.random.split(jax.random.key(seed), 15)
    tokens = centred(arg_keys[0], (SEQS, LENGTH, D), 1.0, 6.0, ((1, 32),))
    norm_gain = jnp.clip(1.0 + 0.18 * jax.random.normal(arg_keys[1], (D,), jnp.float32), 0.1, 1.9)
    x_weight = centred(arg_keys[2], (D, INNER), D ** -0.5, 0.1875, ((0, 8), (1, 4)))
    z_weight = centred(arg_keys[3], (D, INNER), D ** -0.5, 0.1875, ((0, 8), (1, 4)))
    b_weight = centred(arg_keys[4], (D, GROUPS * STATE), D ** -0.5, 0.1875, ((0, 8), (1, 4)))
    c_weight = centred(arg_keys[5], (D, GROUPS * STATE), D ** -0.5, 0.1875, ((0, 8), (1, 4)))
    dt_weight = centred(arg_keys[6], (D, HEADS), D ** -0.5, 0.1875, ((0, 8), (1, 4)))
    x_conv = centred(arg_keys[7], (CONV, INNER), CONV ** -0.5, 3.0, ((1, 4),), jnp.float32)
    b_conv = centred(arg_keys[8], (CONV, GROUPS * STATE), CONV ** -0.5, 3.0, ((1, 4),), jnp.float32)
    c_conv = centred(arg_keys[9], (CONV, GROUPS * STATE), CONV ** -0.5, 3.0, ((1, 4),), jnp.float32)
    dt_bias = jnp.clip(jax.random.uniform(arg_keys[10], (HEADS,), jnp.float32, -1.0, 1.0) * shard_levels(arg_keys[10], (HEADS,), ((0, 4),), -0.4, 0.0), -1.0, 1.0)
    decay_rate = jnp.clip(jnp.exp(math.log(3.5) - 3.149883 * jax.random.uniform(arg_keys[11], (HEADS,), jnp.float32) ** shard_levels(arg_keys[11], (HEADS,), ((0, 4),), -0.2, 0.2)), 0.15, 3.5)
    out_gain = jnp.clip(1.0 + 0.18 * jax.random.normal(arg_keys[12], (INNER,), jnp.float32), 0.1, 1.9)
    out_weight = centred(arg_keys[13], (INNER, D), INNER ** -0.5, 0.1875, ((0, 4), (1, 8)))
    return dict(tokens=tokens, norm_gain=norm_gain, x_weight=x_weight, z_weight=z_weight, b_weight=b_weight, c_weight=c_weight, dt_weight=dt_weight, x_conv=x_conv, b_conv=b_conv, c_conv=c_conv, dt_bias=dt_bias, decay_rate=decay_rate, out_gain=out_gain, out_weight=out_weight)


epsilon = 1e-05
precise = lax.Precision.HIGHEST

def short_conv(projected, taps):
    tap_count = taps.shape[0]
    source = projected.astype(jnp.float32)
    padded = jnp.pad(source, ((0, 0), (tap_count - 1, 0), (0, 0)))
    span_len = source.shape[1]
    running = jnp.zeros_like(source)
    for offset in range(tap_count):
        running = running + taps[offset] * padded[:, offset:offset + span_len]
    return jax.nn.silu(running)

def block_pass(inputs_dt, logdecay, b_state, c_state, per_group):
    seq_count, span_len, head_count, head_width = inputs_dt.shape
    groups, state_width = (b_state.shape[2], b_state.shape[3])
    blocks = span_len // BLOCK
    x_blocks = inputs_dt.reshape(seq_count, blocks, BLOCK, groups, per_group, head_width)
    b_blocks = b_state.reshape(seq_count, blocks, BLOCK, groups, state_width)
    c_blocks = c_state.reshape(seq_count, blocks, BLOCK, groups, state_width)
    log_blocks = logdecay.reshape(seq_count, blocks, BLOCK, groups, per_group)
    within = jnp.moveaxis(jnp.cumsum(log_blocks, axis=2), 2, -1)
    scores = jnp.einsum('sclgn,scmgn->scglm', c_blocks, b_blocks, precision=precise)
    lower_mask = jnp.tril(jnp.ones((BLOCK, BLOCK), dtype=bool))
    log_gaps = jnp.where(lower_mask, within[..., :, None] - within[..., None, :], -jnp.inf)
    weights = scores[:, :, :, None] * jnp.exp(log_gaps)
    diagonal_part = jnp.einsum('scghlm,scmghp->sclghp', weights, x_blocks, precision=precise)
    end_decay = jnp.moveaxis(jnp.exp(within[..., -1:] - within), -1, 2)
    block_states = jnp.einsum('sclgn,sclghp->scghpn', b_blocks, x_blocks * end_decay[..., None], precision=precise)
    block_decay = jnp.exp(within[..., -1])

    def advance(running_state, inputs):
        fresh_state, shrink = inputs
        return (running_state * shrink[..., None, None] + fresh_state, running_state)
    start_state = jnp.zeros((seq_count, groups, per_group, head_width, state_width), jnp.float32)
    final_state, entering = lax.scan(advance, start_state, (jnp.moveaxis(block_states, 1, 0), jnp.moveaxis(block_decay, 1, 0)))
    entering = jnp.moveaxis(entering, 0, 1)
    start_decay = jnp.moveaxis(jnp.exp(within), -1, 2)
    carried_part = jnp.einsum('sclgn,scghpn->sclghp', c_blocks, entering, precision=precise) * start_decay[..., None]
    return ((diagonal_part + carried_part).reshape(seq_count, span_len, head_count, head_width), final_state)

def reference(tokens, norm_gain, x_weight, z_weight, b_weight, c_weight, dt_weight, x_conv, b_conv, c_conv, dt_bias, decay_rate, out_gain, out_weight):
    source = tokens.astype(jnp.float32)
    normed = (source * lax.rsqrt(lax.optimization_barrier(jnp.mean(source * source, axis=-1, keepdims=True)) + epsilon) * norm_gain).astype(jnp.bfloat16)
    flattened = normed.reshape(SEQS * LENGTH, D)

    def project(weight):
        product = jnp.dot(flattened, weight, preferred_element_type=jnp.float32)
        return product.astype(jnp.bfloat16).reshape(SEQS, LENGTH, weight.shape[1])
    x_conv_out = short_conv(project(x_weight), x_conv).reshape(SEQS, LENGTH, HEADS, HEAD_P)
    b_state = short_conv(project(b_weight), b_conv).reshape(SEQS, LENGTH, GROUPS, STATE)
    c_state = short_conv(project(c_weight), c_conv).reshape(SEQS, LENGTH, GROUPS, STATE)
    z_proj = project(z_weight)
    step_dt = jax.nn.softplus(project(dt_weight).astype(jnp.float32) + dt_bias)
    logdecay = -(step_dt * decay_rate) / LENGTH
    y_all, final_state = block_pass(x_conv_out * step_dt[..., None], logdecay, b_state, c_state, HEADS // GROUPS)
    gate_act = jax.nn.silu(z_proj.astype(jnp.float32))
    gated = (y_all.reshape(SEQS, LENGTH, INNER) * gate_act).reshape(SEQS, LENGTH, GROUPS, INNER // GROUPS)
    gated = gated * lax.rsqrt(lax.optimization_barrier(jnp.mean(gated * gated, axis=-1, keepdims=True)) + epsilon)
    gated = (gated.reshape(SEQS, LENGTH, INNER) * out_gain).astype(jnp.bfloat16)
    mixed = jnp.dot(gated.reshape(SEQS * LENGTH, INNER), out_weight, preferred_element_type=jnp.float32)
    return mixed.astype(jnp.bfloat16).reshape(SEQS, LENGTH, D)
```

```python
import functools

import jax
import jax.numpy as jnp
from jax import lax
from jax.experimental import pallas as pl
from jax.experimental.pallas import tpu as pltpu
from jax.sharding import PartitionSpec as P

HEADS = 16
HEAD_P = 64
STATE = 128
GROUPS = 8
CONV = 4
PER_GROUP = HEADS // GROUPS
GROUP_W = PER_GROUP * HEAD_P
LANES = 128
TILE = 16
epsilon = 1e-05
MESH = pl.DeviceIdType.MESH
f32 = jnp.float32
bf16 = jnp.bfloat16


def inner_factor(n):
    best = 1
    for d in range(1, n + 1):
        if n % d == 0 and d * d <= n:
            best = d
    return best


def silu(v):
    return v / (1.0 + jnp.exp(-v))


def expand(cols, group):
    first = group * PER_GROUP
    rows = cols.shape[0]
    lane = lax.broadcasted_iota(jnp.int32, (rows, GROUP_W), 1)
    wide = jnp.broadcast_to(cols[:, first : first + 1], (rows, GROUP_W))
    for k in range(1, PER_GROUP):
        wide = jnp.where(lane >= k * HEAD_P, cols[:, first + k : first + k + 1], wide)
    return wide


class Gather:
    def __init__(self, axis, n, own, slot, send, recv):
        self.axis, self.n, self.own, self.slot = axis, n, own, slot
        self.send, self.recv = send, recv
        self.inner = inner_factor(n)
        self.line = n // self.inner
        me = lax.axis_index(axis)
        self.me, self.a, self.b = me, me // self.inner, me % self.inner

    def target(self, index):
        if self.axis == "sp":
            return (index, lax.axis_index("tp"))
        return (lax.axis_index("sp"), index)

    def copy(self, j, way, index, own=False):
        return pltpu.make_async_remote_copy(
            src_ref=self.own if own else self.slot(j),
            dst_ref=self.slot(j),
            send_sem=self.send.at[j, way],
            recv_sem=self.recv.at[j],
            device_id=self.target(index),
            device_id_type=MESH,
        )

    def sends(self, j, right, left, do, own):
        if right is not None:

            @pl.when(right)
            def _():
                do(self.copy(j, 0, self.me + self.inner, own))

        if left is not None:

            @pl.when(left)
            def _():
                do(self.copy(j, 1, self.me - self.inner, own))

        for k in range(1, self.inner):
            do(self.copy(j, 1 + k, self.a * self.inner + (self.b + k) % self.inner, own))

    def start(self):
        self.sends(self.me, self.a + 1 < self.line, self.a >= 1, lambda c: c.start(), True)

    def each(self, d, do, wait):
        @pl.when(self.a >= d)
        def _():
            j = self.me - d * self.inner
            if wait:
                self.copy(j, 0, j).wait_recv()
            self.sends(j, self.a + 1 < self.line, None, do, False)

        @pl.when(self.a + d < self.line)
        def _():
            j = self.me + d * self.inner
            if wait:
                self.copy(j, 0, j).wait_recv()
            self.sends(j, None, self.a >= 1, do, False)

    def relay(self, d):
        self.each(d, lambda c: c.start(), True)

    def finish(self):
        for k in range(1, self.inner):
            b = (self.b + k) % self.inner
            for a in range(self.line):
                j = a * self.inner + b
                self.copy(j, 0, j).wait_recv()

    def drain(self):
        self.sends(self.me, self.a + 1 < self.line, self.a >= 1, lambda c: c.wait_send(), True)
        for d in range(1, self.line):
            self.each(d, lambda c: c.wait_send(), False)


def kernel(
    sp, tp, seqs, own_len, inner_dev, state_dev,
    tokens, norm_gain, weights, taps, dt_bias, decay_rate, out_gain, out_weight,
    out,
    wbuf, nbuf, wo, proj, halo, ext, bcb, xdt, cums, crow, ybuf, states, pin, pout, gated, gbuf, full,
    w_send, w_recv, n_send, n_recv, o_send, o_recv, q_send, q_recv,
    h_sem, s_send, s_recv, c_send, c_recv, g_send, g_recv,
):
    spi, tpi = lax.axis_index("sp"), lax.axis_index("tp")
    d_model = tokens.shape[2]
    span = own_len * tp
    groups = state_dev // STATE
    conv_w = inner_dev + 2 * state_dev
    krows = weights.shape[0]
    own_rows = seqs * own_len
    length = span * sp

    barrier = pltpu.get_barrier_semaphore()
    for k in range(1, sp):
        pl.semaphore_signal(barrier, inc=1, device_id=((spi + k) % sp, tpi), device_id_type=MESH)
    for k in range(1, tp):
        pl.semaphore_signal(barrier, inc=1, device_id=(spi, (tpi + k) % tp), device_id_type=MESH)
    pl.semaphore_wait(barrier, sp - 1 + tp - 1)

    def rows_of(ref, j, size):
        return ref.at[pl.ds(pl.multiple_of(j * size, size), size), :]

    wg = Gather("sp", sp, weights, lambda j: rows_of(wbuf, j, krows), w_send, w_recv)
    wg.start()

    def norm_one(s, carry):
        src = tokens[s].astype(f32)
        scale = lax.rsqrt(jnp.mean(src * src, axis=-1, keepdims=True) + epsilon)
        at = pl.multiple_of(tpi * own_rows + s * own_len, own_len)
        nbuf[pl.ds(at, own_len), :] = (src * scale * norm_gain[...]).astype(bf16)
        return carry

    lax.fori_loop(0, seqs, norm_one, 0)
    ng = Gather("tp", tp, rows_of(nbuf, tpi, own_rows), lambda j: rows_of(nbuf, j, own_rows), n_send, n_recv)
    ng.start()
    wbuf[pl.ds(pl.multiple_of(spi * krows, krows), krows), :] = weights[...]
    wo[tpi, spi] = out_weight[...]
    og = Gather("sp", sp, out_weight, lambda j: wo.at[tpi, j], o_send, o_recv)
    qg = Gather("tp", tp, wo.at[tpi], lambda j: wo.at[j], q_send, q_recv)
    for d in range(1, max(wg.line, ng.line)):
        if d < wg.line:
            wg.relay(d)
        if d < ng.line:
            ng.relay(d)
    og.start()
    ng.finish()
    wg.finish()

    step_n = 2 * LANES
    cols = wbuf.shape[1]

    def project(i, carry):
        block = nbuf[pl.ds(pl.multiple_of(i * own_rows, own_rows), own_rows), :]
        for lo in range(0, cols, step_n):
            hi = min(cols, lo + step_n)
            res = jnp.dot(block, wbuf[:, lo:hi], preferred_element_type=f32).astype(bf16)
            for s in range(seqs):
                at = pl.multiple_of(s * span + i * own_len, own_len)
                proj[pl.ds(at, own_len), lo:hi] = res[s * own_len : (s + 1) * own_len]
        return carry

    lax.fori_loop(0, tp, project, 0)

    def halo_copy(s):
        return pltpu.make_async_remote_copy(
            src_ref=proj.at[pl.ds(s * span + span - TILE, TILE), pl.ds(0, conv_w)],
            dst_ref=halo.at[s],
            send_sem=h_sem.at[0, s],
            recv_sem=h_sem.at[1, s],
            device_id=(lax.rem(spi + 1, sp), tpi),
            device_id_type=MESH,
        )

    @pl.when(spi + 1 < sp)
    def _():
        for s in range(seqs):
            halo_copy(s).start()

    if og.line > 1:
        og.relay(1)

    row_i = lax.broadcasted_iota(jnp.int32, (span, span), 0)
    col_i = lax.broadcasted_iota(jnp.int32, (span, span), 1)
    lower = (row_i >= col_i).astype(f32)
    upper = (row_i <= col_i).astype(f32)

    def decay_of(s, carry):
        at = pl.ds(pl.multiple_of(s * span, span), span)
        raw = proj[at, conv_w + inner_dev :].astype(f32) + dt_bias[...]
        dt = jnp.maximum(raw, 0.0) + jnp.log1p(jnp.exp(-jnp.abs(raw)))
        log = -(dt * decay_rate[...]) / length
        cums[at, :LANES] = dt
        cums[at, LANES:] = jnp.dot(lower, log, preferred_element_type=f32, precision=lax.Precision.HIGHEST)
        across = lax.dot_general(
            log, upper, (((0,), (0,)), ((), ())),
            preferred_element_type=f32, precision=lax.Precision.HIGHEST,
        )
        crow[s] = across[:8]
        return carry

    lax.fori_loop(0, seqs, decay_of, 0)

    for d in range(2, og.line):
        og.relay(d)

    @pl.when(spi >= 1)
    def _():
        for s in range(seqs):
            halo_copy(s).wait_recv()

    @pl.when(spi == 0)
    def _():
        halo[...] = jnp.zeros_like(halo)

    gin = inner_factor(sp)
    line = sp // gin
    za, zb = spi // gin, spi % gin

    def peer_copy(s, b, k):
        return pltpu.make_async_remote_copy(
            src_ref=states.at[b, s],
            dst_ref=states.at[b, s],
            send_sem=s_send.at[s, k],
            recv_sem=s_recv.at[b, s],
            device_id=(za * gin + (zb + k) % gin, tpi),
            device_id_type=MESH,
        )

    def local(s, carry):
        at = pl.ds(pl.multiple_of(s * span, span), span)
        for lo in range(0, conv_w, LANES):
            part = slice(lo, lo + LANES)
            ext[0:TILE, part] = halo[s, :, part].astype(f32)
            ext[TILE:, part] = proj[at, part].astype(f32)
        dt = cums[at, :LANES]
        cum = cums[at, LANES:]

        def conv(lo):
            part = slice(lo, lo + LANES)
            total = taps[0:1, part] * ext[TILE - CONV + 1 : TILE - CONV + 1 + span, part]
            for k in range(1, CONV):
                begin = TILE - CONV + 1 + k
                total = total + taps[k : k + 1, part] * ext[begin : begin + span, part]
            return silu(total)

        for g in range(groups):
            xd = conv(g * GROUP_W) * expand(dt, g)
            bg = conv(inner_dev + g * STATE).astype(bf16)
            cg = conv(inner_dev + state_dev + g * STATE).astype(bf16)
            wide = expand(cum, g)
            last = wide[span - 1 : span, :]
            xdt[at, g * GROUP_W : (g + 1) * GROUP_W] = xd.astype(bf16)
            bcb[at, g * STATE : (g + 1) * STATE] = bg
            bcb[at, state_dev + g * STATE : state_dev + (g + 1) * STATE] = cg
            st = lax.dot_general(
                bg, (xd * jnp.exp(last - wide)).astype(bf16), (((0,), (0,)), ((), ())),
                preferred_element_type=f32,
            )
            states[zb, s, g * STATE : (g + 1) * STATE, :] = st.astype(bf16)
            fade_at = groups * STATE + g * TILE
            states[zb, s, fade_at : fade_at + TILE, :] = (
                jnp.broadcast_to(jnp.exp(last), (TILE, GROUP_W)).astype(bf16)
            )
        for k in range(1, gin):
            peer_copy(s, zb, k).start()
        return carry

    lax.fori_loop(0, seqs, local, 0)
    og.finish()
    qg.start()

    def chain_copy(s):
        return pltpu.make_async_remote_copy(
            src_ref=pout.at[s],
            dst_ref=pin.at[s],
            send_sem=c_send.at[s],
            recv_sem=c_recv.at[s],
            device_id=(lax.rem(spi + gin, sp), tpi),
            device_id_type=MESH,
        )

    def chain(s):
        for k in range(1, gin):
            peer_copy(s, (zb + k) % gin, k).wait_recv()

        @pl.when(za == 0)
        def _():
            pin[s] = jnp.zeros(pin.shape[1:], bf16)

        @pl.when(za >= 1)
        def _():
            chain_copy(s).wait_recv()

        for g in range(groups):
            part = slice(g * STATE, (g + 1) * STATE)
            total = pin[s, part, :].astype(f32)
            mine = total
            for b in range(gin):
                mine = jnp.where(zb == b, total, mine)
                fade = states[b, s, groups * STATE + g * TILE : groups * STATE + (g + 1) * TILE, :].astype(f32)
                total = total * fade[0:1, :] + states[b, s, part, :].astype(f32)
            pout[s, part, :] = total.astype(bf16)
            full[s, part, :] = mine.astype(bf16)

        @pl.when(za + 1 < line)
        def _():
            chain_copy(s).start()

    def diagonal(s):
        at = pl.ds(pl.multiple_of(s * span, span), span)
        cum = cums[at, LANES:]
        lane = lax.broadcasted_iota(jnp.int32, (span, GROUP_W), 1)
        mask = lax.broadcasted_iota(jnp.int32, (span, span), 0) >= lax.broadcasted_iota(jnp.int32, (span, span), 1)
        for g in range(groups):
            bg = bcb[at, g * STATE : (g + 1) * STATE]
            cg = bcb[at, state_dev + g * STATE : state_dev + (g + 1) * STATE]
            xg = xdt[at, g * GROUP_W : (g + 1) * GROUP_W]
            scores = lax.dot_general(cg, bg, (((1,), (1,)), ((), ())), preferred_element_type=f32)
            yg = None
            for k in range(PER_GROUP):
                h = g * PER_GROUP + k
                gaps = jnp.where(mask, cum[:, h : h + 1] - crow[s, h : h + 1, :], -jnp.inf)
                part = jnp.dot((scores * jnp.exp(gaps)).astype(bf16), xg, preferred_element_type=f32)
                yg = part if yg is None else jnp.where(lane >= k * HEAD_P, part, yg)
            ybuf[at, g * GROUP_W : (g + 1) * GROUP_W] = yg

    def steps(t, carry):
        @pl.when((t >= za) & (t - za < seqs))
        def _():
            chain(t - za)

        @pl.when(t < seqs)
        def _():
            diagonal(t)

        return carry

    lax.fori_loop(0, seqs + line - 1, steps, 0)
    for d in range(1, qg.line):
        qg.relay(d)

    def a2a_copy(s, k):
        to = (tpi + k) % tp
        return pltpu.make_async_remote_copy(
            src_ref=gated.at[pl.ds(pl.multiple_of(s * span + to * own_len, own_len), own_len), :],
            dst_ref=gbuf.at[tpi, pl.ds(pl.multiple_of(s * own_len, own_len), own_len), :],
            send_sem=g_send.at[s, k],
            recv_sem=g_recv.at[tpi, s],
            device_id=(spi, to),
            device_id_type=MESH,
        )

    def a2a_wait(s, k):
        frm = (tpi + k) % tp
        pltpu.make_async_remote_copy(
            src_ref=gated.at[pl.ds(0, own_len), :],
            dst_ref=gbuf.at[frm, pl.ds(pl.multiple_of(s * own_len, own_len), own_len), :],
            send_sem=g_send.at[s, k],
            recv_sem=g_recv.at[frm, s],
            device_id=(spi, frm),
            device_id_type=MESH,
        ).wait_recv()

    def finish(s, carry):
        at = pl.ds(pl.multiple_of(s * span, span), span)
        cum = cums[at, LANES:]
        for g in range(groups):
            part = slice(g * GROUP_W, (g + 1) * GROUP_W)
            cg = bcb[at, state_dev + g * STATE : state_dev + (g + 1) * STATE]
            carried = jnp.dot(cg, full[s, g * STATE : (g + 1) * STATE, :], preferred_element_type=f32)
            y = ybuf[at, part] + carried * jnp.exp(expand(cum, g))
            z = proj[at, conv_w + g * GROUP_W : conv_w + (g + 1) * GROUP_W].astype(f32)
            v = y * silu(z)
            v = v * lax.rsqrt(jnp.mean(v * v, axis=-1, keepdims=True) + epsilon)
            gated[at, part] = (v * out_gain[:, part]).astype(bf16)
        for k in range(1, tp):
            a2a_copy(s, k).start()
        own_at = pl.multiple_of(s * span + tpi * own_len, own_len)
        gbuf[tpi, pl.ds(pl.multiple_of(s * own_len, own_len), own_len), :] = gated[pl.ds(own_at, own_len), :]
        return carry

    lax.fori_loop(0, seqs, finish, 0)
    qg.finish()
    for s in range(seqs):
        for k in range(1, tp):
            a2a_wait(s, k)

    width = out_weight.shape[1]
    for j in range(sp):
        total = jnp.dot(gbuf[0], wo[0, j], preferred_element_type=f32)
        for i in range(1, tp):
            total = total + jnp.dot(gbuf[i], wo[i, j], preferred_element_type=f32)
        res = total.astype(bf16)
        for s in range(seqs):
            out[s, :, j * width : (j + 1) * width] = res[s * own_len : (s + 1) * own_len]

    for gather in (wg, ng, og, qg):
        gather.drain()
    for s in range(seqs):
        for k in range(1, gin):
            peer_copy(s, zb, k).wait_send()
        for k in range(1, tp):
            a2a_copy(s, k).wait_send()

    @pl.when(spi + 1 < sp)
    def _():
        for s in range(seqs):
            halo_copy(s).wait_send()

    @pl.when(za + 1 < line)
    def _():
        for s in range(seqs):
            chain_copy(s).wait_send()


def pad_lanes(a):
    return jnp.pad(a, ((0, 0), (0, LANES - a.shape[1])))


def on_device(
    sp, tp, tokens, norm_gain, x_weight, z_weight, b_weight, c_weight, dt_weight,
    x_conv, b_conv, c_conv, dt_bias, decay_rate, out_gain, out_weight,
):
    seqs, own_len, d_model = tokens.shape
    inner_dev, state_dev = x_weight.shape[1], b_weight.shape[1]
    groups = state_dev // STATE
    span = own_len * tp
    rows = seqs * span
    weights = jnp.concatenate([x_weight, b_weight, c_weight, z_weight, pad_lanes(dt_weight)], axis=1)
    taps = jnp.concatenate([x_conv, b_conv, c_conv], axis=1)
    cols = weights.shape[1]
    conv_w = inner_dev + 2 * state_dev
    gin = inner_factor(sp)
    vmem = pl.BlockSpec(memory_space=pltpu.VMEM)
    dma = pltpu.SemaphoreType.DMA

    def gather_sems(n):
        return [dma((n, 1 + max(inner_factor(n), 1))), dma((n,))]

    return pl.pallas_call(
        functools.partial(kernel, sp, tp, seqs, own_len, inner_dev, state_dev),
        out_shape=jax.ShapeDtypeStruct(tokens.shape, bf16),
        in_specs=[vmem] * 8,
        out_specs=vmem,
        scratch_shapes=[
            pltpu.VMEM((d_model, cols), bf16),
            pltpu.VMEM((rows, d_model), bf16),
            pltpu.VMEM((tp, sp) + out_weight.shape, bf16),
            pltpu.VMEM((rows, cols), bf16),
            pltpu.VMEM((seqs, TILE, conv_w), bf16),
            pltpu.VMEM((TILE + span, conv_w), f32),
            pltpu.VMEM((rows, 2 * state_dev), bf16),
            pltpu.VMEM((rows, inner_dev), bf16),
            pltpu.VMEM((rows, 2 * LANES), f32),
            pltpu.VMEM((seqs, 8, span), f32),
            pltpu.VMEM((rows, inner_dev), f32),
            pltpu.VMEM((gin, seqs, groups * (STATE + TILE), GROUP_W), bf16),
            pltpu.VMEM((seqs, groups * STATE, GROUP_W), bf16),
            pltpu.VMEM((seqs, groups * STATE, GROUP_W), bf16),
            pltpu.VMEM((rows, inner_dev), bf16),
            pltpu.VMEM((tp, seqs * own_len, inner_dev), bf16),
            pltpu.VMEM((seqs, groups * STATE, GROUP_W), bf16),
            *gather_sems(sp), *gather_sems(tp), *gather_sems(sp), *gather_sems(tp),
            dma((2, seqs)),
            dma((seqs, gin)), dma((gin, seqs)),
            dma((seqs,)), dma((seqs,)),
            dma((seqs, tp)), dma((tp, seqs)),
        ],
        compiler_params=pltpu.CompilerParams(
            collective_id=0, has_side_effects=True, vmem_limit_bytes=56 * 2**20
        ),
    )(
        tokens, norm_gain[None, :], weights, taps, pad_lanes(dt_bias[None, :]),
        pad_lanes(decay_rate[None, :]), out_gain[None, :], out_weight,
    )


def solution(mesh):
    return jax.shard_map(
        functools.partial(on_device, mesh.shape["sp"], mesh.shape["tp"]),
        mesh=mesh,
        in_specs=(
            P(None, ("sp", "tp"), None),
            P(),
            P("sp", "tp"),
            P("sp", "tp"),
            P("sp", "tp"),
            P("sp", "tp"),
            P("sp", "tp"),
            P(None, "tp"),
            P(None, "tp"),
            P(None, "tp"),
            P("tp"),
            P("tp"),
            P("tp"),
            P("tp", "sp"),
        ),
        out_specs=P(None, ("sp", "tp"), None),
        check_vma=False,
    )
```

```python
import functools

import jax
import jax.numpy as jnp
from jax import lax
from jax.experimental import pallas as pl
from jax.experimental.pallas import tpu as pltpu
from jax.sharding import PartitionSpec as P

HEADS = 16
HEAD_P = 64
STATE = 128
GROUPS = 8
CONV = 4
PER_GROUP = HEADS // GROUPS
GROUP_W = PER_GROUP * HEAD_P
LANES = 128
TILE = 16
epsilon = 1e-05
MESH = pl.DeviceIdType.MESH
f32 = jnp.float32
bf16 = jnp.bfloat16


def inner_factor(n):
    best = 1
    for d in range(1, n + 1):
        if n % d == 0 and d * d <= n:
            best = d
    return best


def silu(v):
    return v / (1.0 + jnp.exp(-v))


def expand(cols, group):
    first = group * PER_GROUP
    rows = cols.shape[0]
    lane = lax.broadcasted_iota(jnp.int32, (rows, GROUP_W), 1)
    wide = jnp.broadcast_to(cols[:, first : first + 1], (rows, GROUP_W))
    for k in range(1, PER_GROUP):
        wide = jnp.where(lane >= k * HEAD_P, cols[:, first + k : first + k + 1], wide)
    return wide


class Gather:
    def __init__(self, axis, n, own, slot, send, recv):
        self.axis, self.n, self.own, self.slot = axis, n, own, slot
        self.send, self.recv = send, recv
        self.inner = inner_factor(n)
        self.line = n // self.inner
        me = lax.axis_index(axis)
        self.me, self.a, self.b = me, me // self.inner, me % self.inner

    def target(self, index):
        if self.axis == "sp":
            return (index, lax.axis_index("tp"))
        return (lax.axis_index("sp"), index)

    def copy(self, j, way, index, own=False):
        return pltpu.make_async_remote_copy(
            src_ref=self.own if own else self.slot(j),
            dst_ref=self.slot(j),
            send_sem=self.send.at[j, way],
            recv_sem=self.recv.at[j],
            device_id=self.target(index),
            device_id_type=MESH,
        )

    def sends(self, j, right, left, do, own, peers=True):
        if right is not None:

            @pl.when(right)
            def _():
                do(self.copy(j, 0, self.me + self.inner, own))

        if left is not None:

            @pl.when(left)
            def _():
                do(self.copy(j, 1, self.me - self.inner, own))

        if peers:
            self.to_peers(j, do, own)

    def to_peers(self, j, do, own):
        for k in range(1, self.inner):
            do(self.copy(j, 1 + k, self.a * self.inner + (self.b + k) % self.inner, own))

    def start(self, peers=True):
        self.sends(self.me, self.a + 1 < self.line, self.a >= 1, lambda c: c.start(), True, peers)

    def pass_on(self):
        self.to_peers(self.me, lambda c: c.start(), True)
        for d in range(1, self.line):
            j = (self.a + d) % self.line * self.inner + self.b
            self.to_peers(j, lambda c: c.start(), False)

    def each(self, d, do, wait, peers=True):
        @pl.when(self.a >= d)
        def _():
            j = self.me - d * self.inner
            if wait:
                self.copy(j, 0, j).wait_recv()
            self.sends(j, self.a + 1 < self.line, None, do, False, peers)

        @pl.when(self.a + d < self.line)
        def _():
            j = self.me + d * self.inner
            if wait:
                self.copy(j, 0, j).wait_recv()
            self.sends(j, None, self.a >= 1, do, False, peers)

    def relay(self, d, peers=True):
        self.each(d, lambda c: c.start(), True, peers)

    def finish(self):
        for k in range(1, self.inner):
            b = (self.b + k) % self.inner
            for a in range(self.line):
                j = a * self.inner + b
                self.copy(j, 0, j).wait_recv()

    def drain(self):
        self.sends(self.me, self.a + 1 < self.line, self.a >= 1, lambda c: c.wait_send(), True)
        for d in range(1, self.line):
            self.each(d, lambda c: c.wait_send(), False)


def kernel(
    sp, tp, seqs, own_len, inner_dev, state_dev,
    tokens_in, norm_gain_in, x_weight, z_weight, b_weight, c_weight, dt_weight,
    x_conv, b_conv, c_conv, dt_bias_in, decay_rate_in, out_gain_in, out_weight_in,
    out,
    tokens, norm_gain, taps, dt_w, dt_bias, decay_rate, out_gain, out_weight, in_sem,
    wbuf, dtb, dtall, nbuf, wo, proj, halo, ext, bcb, xdt, cums, crow, ybuf, states, pin, pout, gated, gbuf, full,
    w_send, w_recv, d_send, d_recv, n_send, n_recv, o_send, o_recv, q_send, q_recv,
    h_sem, s_send, s_recv, c_send, c_recv, g_send, g_recv,
):
    spi, tpi = lax.axis_index("sp"), lax.axis_index("tp")
    d_model = tokens.shape[2]
    span = own_len * tp
    groups = state_dev // STATE
    conv_w = inner_dev + 2 * state_dev
    krows = x_weight.shape[0]
    heads_dev = dt_weight.shape[0]
    own_rows = seqs * own_len
    length = span * sp

    def rows_of(ref, j, size):
        return ref.at[pl.ds(pl.multiple_of(j * size, size), size), :]

    own_w = rows_of(wbuf, spi, krows)
    own_at = pl.ds(pl.multiple_of(spi * krows, krows), krows)
    moves = [(dt_weight, dt_w)]
    at = 0
    for ref in (x_weight, b_weight, c_weight, z_weight):
        moves.append((ref, wbuf.at[own_at, pl.ds(at, ref.shape[1])]))
        at += ref.shape[1]
    early = len(moves)
    moves += [(tokens_in, tokens), (norm_gain_in, norm_gain), (out_weight_in, out_weight)]
    middle = len(moves)
    at = 0
    for ref in (x_conv, b_conv, c_conv):
        moves.append((ref, taps.at[:, pl.ds(at, ref.shape[1])]))
        at += ref.shape[1]
    moves += [(dt_bias_in, dt_bias), (decay_rate_in, decay_rate), (out_gain_in, out_gain)]
    loads = [pltpu.make_async_copy(a, b, in_sem.at[k]) for k, (a, b) in enumerate(moves)]
    for load in loads:
        load.start()

    barrier = pltpu.get_barrier_semaphore()
    for k in range(1, sp):
        pl.semaphore_signal(barrier, inc=1, device_id=((spi + k) % sp, tpi), device_id_type=MESH)
    for k in range(1, tp):
        pl.semaphore_signal(barrier, inc=1, device_id=(spi, (tpi + k) % tp), device_id_type=MESH)
    for load in loads[:early]:
        load.wait()
    main_w = inner_dev * 2 + state_dev * 2
    pl.semaphore_wait(barrier, sp - 1 + tp - 1)
    wg = Gather("sp", sp, own_w, lambda j: rows_of(wbuf, j, krows), w_send, w_recv)
    dg = Gather("sp", sp, dt_w, lambda j: dtb.at[j], d_send, d_recv)
    dg.start()
    wg.start()
    dtb[spi] = dt_w[...]
    for load in loads[early:middle]:
        load.wait()

    def norm_one(s, carry):
        src = tokens[s].astype(f32)
        scale = lax.rsqrt(jnp.mean(src * src, axis=-1, keepdims=True) + epsilon)
        at = pl.multiple_of(tpi * own_rows + s * own_len, own_len)
        nbuf[pl.ds(at, own_len), :] = (src * scale * norm_gain[...]).astype(bf16)
        return carry

    lax.fori_loop(0, seqs, norm_one, 0)
    ng = Gather("tp", tp, rows_of(nbuf, tpi, own_rows), lambda j: rows_of(nbuf, j, own_rows), n_send, n_recv)
    ng.start()
    wo[tpi, spi] = out_weight[...]
    og = Gather("sp", sp, out_weight, lambda j: wo.at[tpi, j], o_send, o_recv)

    def qg(j):
        return Gather("tp", tp, wo.at[tpi, j], lambda i: wo.at[i, j], q_send.at[j], q_recv.at[j])

    def q_each(own_peer, do):
        gin = og.inner

        def one(t, carry):
            if own_peer:
                do(qg(t * gin + og.b))
            else:
                for k in range(1, gin):
                    do(qg(t * gin + (og.b + k) % gin))
            return carry

        lax.fori_loop(0, og.line, one, 0)

    def q_relay(q):
        for d in range(1, q.line):
            q.relay(d)

    og.start(peers=False)
    for d in range(1, max(wg.line, ng.line)):
        if d < wg.line:
            dg.relay(d)
            wg.relay(d)
            og.relay(d, peers=False)
        if d < ng.line:
            ng.relay(d)
    og.pass_on()
    q_each(True, lambda q: q.start())
    for load in loads[middle:]:
        load.wait()
    ng.finish()
    wg.finish()
    dg.finish()

    step_n = 2 * LANES
    for j in range(sp):
        dtall[:heads_dev, j * krows : (j + 1) * krows] = dtb[j]
    cols = wbuf.shape[1]

    def project(i, carry):
        block = nbuf[pl.ds(pl.multiple_of(i * own_rows, own_rows), own_rows), :]
        for lo in range(0, cols, step_n):
            hi = min(cols, lo + step_n)
            res = jnp.dot(block, wbuf[:, lo:hi], preferred_element_type=f32).astype(bf16)
            for s in range(seqs):
                at = pl.multiple_of(s * span + i * own_len, own_len)
                proj[pl.ds(at, own_len), lo:hi] = res[s * own_len : (s + 1) * own_len]
        res = lax.dot_general(
            block, dtall[...], (((1,), (1,)), ((), ())), preferred_element_type=f32
        ).astype(bf16)
        for s in range(seqs):
            at = pl.multiple_of(s * span + i * own_len, own_len)
            proj[pl.ds(at, own_len), main_w : main_w + heads_dev] = res[s * own_len : (s + 1) * own_len, :heads_dev]
        return carry

    lax.fori_loop(0, tp, project, 0)

    def halo_copy(s):
        return pltpu.make_async_remote_copy(
            src_ref=proj.at[pl.ds(s * span + span - TILE, TILE), pl.ds(0, conv_w)],
            dst_ref=halo.at[s],
            send_sem=h_sem.at[0, s],
            recv_sem=h_sem.at[1, s],
            device_id=(lax.rem(spi + 1, sp), tpi),
            device_id_type=MESH,
        )

    @pl.when(spi + 1 < sp)
    def _():
        for s in range(seqs):
            halo_copy(s).start()

    row_i = lax.broadcasted_iota(jnp.int32, (span, span), 0)
    col_i = lax.broadcasted_iota(jnp.int32, (span, span), 1)
    lower = (row_i >= col_i).astype(f32)
    upper = (row_i <= col_i).astype(f32)

    def decay_of(s, carry):
        at = pl.ds(pl.multiple_of(s * span, span), span)
        raw = proj[at, conv_w + inner_dev : conv_w + inner_dev + heads_dev].astype(f32) + dt_bias[...]
        dt = jnp.maximum(raw, 0.0) + jnp.log1p(jnp.exp(-jnp.abs(raw)))
        log = -(dt * decay_rate[...]) / length
        cums[at, :heads_dev] = dt
        cums[at, LANES : LANES + heads_dev] = jnp.dot(lower, log, preferred_element_type=f32, precision=lax.Precision.HIGHEST)
        across = lax.dot_general(
            log, upper, (((0,), (0,)), ((), ())),
            preferred_element_type=f32, precision=lax.Precision.HIGHEST,
        )
        crow[s, :heads_dev] = across
        return carry

    lax.fori_loop(0, seqs, decay_of, 0)

    @pl.when(spi >= 1)
    def _():
        for s in range(seqs):
            halo_copy(s).wait_recv()

    @pl.when(spi == 0)
    def _():
        halo[...] = jnp.zeros_like(halo)

    gin = inner_factor(sp)
    line = sp // gin
    za, zb = spi // gin, spi % gin

    def peer_copy(s, b, k):
        return pltpu.make_async_remote_copy(
            src_ref=states.at[b, s],
            dst_ref=states.at[b, s],
            send_sem=s_send.at[s, k],
            recv_sem=s_recv.at[b, s],
            device_id=(za * gin + (zb + k) % gin, tpi),
            device_id_type=MESH,
        )

    def local(s, carry):
        at = pl.ds(pl.multiple_of(s * span, span), span)
        for lo in range(0, conv_w, LANES):
            part = slice(lo, lo + LANES)
            ext[0:TILE, part] = halo[s, :, part].astype(f32)
            ext[TILE:, part] = proj[at, part].astype(f32)
        dt = cums[at, :LANES]
        cum = cums[at, LANES:]

        def conv(lo):
            part = slice(lo, lo + LANES)
            total = taps[0:1, part] * ext[TILE - CONV + 1 : TILE - CONV + 1 + span, part]
            for k in range(1, CONV):
                begin = TILE - CONV + 1 + k
                total = total + taps[k : k + 1, part] * ext[begin : begin + span, part]
            return silu(total)

        for g in range(groups):
            xd = conv(g * GROUP_W) * expand(dt, g)
            bg = conv(inner_dev + g * STATE).astype(bf16)
            cg = conv(inner_dev + state_dev + g * STATE).astype(bf16)
            wide = expand(cum, g)
            last = wide[span - 1 : span, :]
            xdt[at, g * GROUP_W : (g + 1) * GROUP_W] = xd.astype(bf16)
            bcb[at, g * STATE : (g + 1) * STATE] = bg
            bcb[at, state_dev + g * STATE : state_dev + (g + 1) * STATE] = cg
            st = lax.dot_general(
                bg, (xd * jnp.exp(last - wide)).astype(bf16), (((0,), (0,)), ((), ())),
                preferred_element_type=f32,
            )
            states[zb, s, g * STATE : (g + 1) * STATE, :] = st.astype(bf16)
            fade_at = groups * STATE + g * TILE
            states[zb, s, fade_at : fade_at + TILE, :] = (
                jnp.broadcast_to(jnp.exp(last), (TILE, GROUP_W)).astype(bf16)
            )
        for k in range(1, gin):
            peer_copy(s, zb, k).start()
        return carry

    lax.fori_loop(0, seqs, local, 0)
    og.finish()
    q_each(False, lambda q: q.start())
    q_each(True, q_relay)

    def chain_copy(s, g):
        part = pl.ds(g * STATE, STATE)
        return pltpu.make_async_remote_copy(
            src_ref=pout.at[s, part, :],
            dst_ref=pin.at[s, part, :],
            send_sem=c_send.at[s, g],
            recv_sem=c_recv.at[s, g],
            device_id=(lax.rem(spi + gin, sp), tpi),
            device_id_type=MESH,
        )

    def chain(s):
        for k in range(1, gin):
            peer_copy(s, (zb + k) % gin, k).wait_recv()

        @pl.when(za == 0)
        def _():
            pin[s] = jnp.zeros(pin.shape[1:], bf16)

        for g in range(groups):
            part = slice(g * STATE, (g + 1) * STATE)

            @pl.when(za >= 1)
            def _():
                chain_copy(s, g).wait_recv()

            total = pin[s, part, :].astype(f32)
            mine = total
            for b in range(gin):
                mine = jnp.where(zb == b, total, mine)
                fade = states[b, s, groups * STATE + g * TILE : groups * STATE + (g + 1) * TILE, :].astype(f32)
                total = total * fade[0:1, :] + states[b, s, part, :].astype(f32)
            pout[s, part, :] = total.astype(bf16)

            @pl.when(za + 1 < line)
            def _():
                chain_copy(s, g).start()

            full[s, part, :] = mine.astype(bf16)

    def diagonal(s):
        at = pl.ds(pl.multiple_of(s * span, span), span)
        cum = cums[at, LANES:]
        lane = lax.broadcasted_iota(jnp.int32, (span, GROUP_W), 1)
        mask = lax.broadcasted_iota(jnp.int32, (span, span), 0) >= lax.broadcasted_iota(jnp.int32, (span, span), 1)
        for g in range(groups):
            bg = bcb[at, g * STATE : (g + 1) * STATE]
            cg = bcb[at, state_dev + g * STATE : state_dev + (g + 1) * STATE]
            xg = xdt[at, g * GROUP_W : (g + 1) * GROUP_W]
            scores = lax.dot_general(cg, bg, (((1,), (1,)), ((), ())), preferred_element_type=f32)
            yg = None
            for k in range(PER_GROUP):
                h = g * PER_GROUP + k
                gaps = jnp.where(mask, cum[:, h : h + 1] - crow[s, h : h + 1, :], -jnp.inf)
                part = jnp.dot((scores * jnp.exp(gaps)).astype(bf16), xg, preferred_element_type=f32)
                yg = part if yg is None else jnp.where(lane >= k * HEAD_P, part, yg)
            ybuf[at, g * GROUP_W : (g + 1) * GROUP_W] = yg

    def steps(t, carry):
        @pl.when((t >= za) & (t - za < seqs))
        def _():
            chain(t - za)

        @pl.when(t < seqs)
        def _():
            diagonal(t)

        return carry

    lax.fori_loop(0, seqs + line - 1, steps, 0)
    q_each(False, q_relay)

    def a2a_copy(s, k):
        to = (tpi + k) % tp
        return pltpu.make_async_remote_copy(
            src_ref=gated.at[pl.ds(pl.multiple_of(s * span + to * own_len, own_len), own_len), :],
            dst_ref=gbuf.at[tpi, pl.ds(pl.multiple_of(s * own_len, own_len), own_len), :],
            send_sem=g_send.at[s, k],
            recv_sem=g_recv.at[tpi, s],
            device_id=(spi, to),
            device_id_type=MESH,
        )

    def a2a_wait(s, k):
        frm = (tpi + k) % tp
        pltpu.make_async_remote_copy(
            src_ref=gated.at[pl.ds(0, own_len), :],
            dst_ref=gbuf.at[frm, pl.ds(pl.multiple_of(s * own_len, own_len), own_len), :],
            send_sem=g_send.at[s, k],
            recv_sem=g_recv.at[frm, s],
            device_id=(spi, frm),
            device_id_type=MESH,
        ).wait_recv()

    def finish(s, carry):
        at = pl.ds(pl.multiple_of(s * span, span), span)
        cum = cums[at, LANES:]
        for g in range(groups):
            part = slice(g * GROUP_W, (g + 1) * GROUP_W)
            cg = bcb[at, state_dev + g * STATE : state_dev + (g + 1) * STATE]
            carried = jnp.dot(cg, full[s, g * STATE : (g + 1) * STATE, :], preferred_element_type=f32)
            y = ybuf[at, part] + carried * jnp.exp(expand(cum, g))
            z = proj[at, conv_w + g * GROUP_W : conv_w + (g + 1) * GROUP_W].astype(f32)
            v = y * silu(z)
            v = v * lax.rsqrt(jnp.mean(v * v, axis=-1, keepdims=True) + epsilon)
            gated[at, part] = (v * out_gain[:, part]).astype(bf16)
        for k in range(1, tp):
            a2a_copy(s, k).start()
        own_at = pl.multiple_of(s * span + tpi * own_len, own_len)
        gbuf[tpi, pl.ds(pl.multiple_of(s * own_len, own_len), own_len), :] = gated[pl.ds(own_at, own_len), :]
        return carry

    lax.fori_loop(0, seqs, finish, 0)
    q_each(True, lambda q: q.finish())
    q_each(False, lambda q: q.finish())
    for s in range(seqs):
        for k in range(1, tp):
            a2a_wait(s, k)

    width = out_weight.shape[1]
    for j in range(sp):
        total = jnp.dot(gbuf[0], wo[0, j], preferred_element_type=f32)
        for i in range(1, tp):
            total = total + jnp.dot(gbuf[i], wo[i, j], preferred_element_type=f32)
        res = total.astype(bf16)
        for s in range(seqs):
            out[s, :, j * width : (j + 1) * width] = res[s * own_len : (s + 1) * own_len]

    for gather in (wg, dg, ng, og):
        gather.drain()
    q_each(True, lambda q: q.drain())
    q_each(False, lambda q: q.drain())
    for s in range(seqs):
        for k in range(1, gin):
            peer_copy(s, zb, k).wait_send()
        for k in range(1, tp):
            a2a_copy(s, k).wait_send()

    @pl.when(spi + 1 < sp)
    def _():
        for s in range(seqs):
            halo_copy(s).wait_send()

    @pl.when(za + 1 < line)
    def _():
        for s in range(seqs):
            for g in range(groups):
                chain_copy(s, g).wait_send()


def on_device(
    sp, tp, tokens, norm_gain, x_weight, z_weight, b_weight, c_weight, dt_weight,
    x_conv, b_conv, c_conv, dt_bias, decay_rate, out_gain, out_weight,
):
    seqs, own_len, d_model = tokens.shape
    inner_dev, state_dev = x_weight.shape[1], b_weight.shape[1]
    groups = state_dev // STATE
    span = own_len * tp
    rows = seqs * span
    cols = 2 * inner_dev + 2 * state_dev
    conv_w = inner_dev + 2 * state_dev
    gin = inner_factor(sp)
    vmem = pl.BlockSpec(memory_space=pltpu.VMEM)
    dma = pltpu.SemaphoreType.DMA

    def gather_sems(n):
        return [dma((n, 1 + max(inner_factor(n), 1))), dma((n,))]

    return pl.pallas_call(
        functools.partial(kernel, sp, tp, seqs, own_len, inner_dev, state_dev),
        out_shape=jax.ShapeDtypeStruct(tokens.shape, bf16),
        in_specs=[pl.BlockSpec(memory_space=pl.ANY)] * 14,
        out_specs=vmem,
        scratch_shapes=[
            pltpu.VMEM(tokens.shape, bf16),
            pltpu.VMEM((1, d_model), f32),
            pltpu.VMEM((x_conv.shape[0], conv_w), f32),
            pltpu.VMEM(dt_weight.shape[::-1], bf16),
            pltpu.VMEM((1, dt_weight.shape[1]), f32),
            pltpu.VMEM((1, dt_weight.shape[1]), f32),
            pltpu.VMEM((1, inner_dev), f32),
            pltpu.VMEM(out_weight.shape, bf16),
            dma((14,)),
            pltpu.VMEM((d_model, cols), bf16),
            pltpu.VMEM((sp,) + dt_weight.shape[::-1], bf16),
            pltpu.VMEM((TILE, d_model), bf16),
            pltpu.VMEM((rows, d_model), bf16),
            pltpu.VMEM((tp, sp) + out_weight.shape, bf16),
            pltpu.VMEM((rows, cols + LANES), bf16),
            pltpu.VMEM((seqs, TILE, conv_w), bf16),
            pltpu.VMEM((TILE + span, conv_w), f32),
            pltpu.VMEM((rows, 2 * state_dev), bf16),
            pltpu.VMEM((rows, inner_dev), bf16),
            pltpu.VMEM((rows, 2 * LANES), f32),
            pltpu.VMEM((seqs, 8, span), f32),
            pltpu.VMEM((rows, inner_dev), f32),
            pltpu.VMEM((gin, seqs, groups * (STATE + TILE), GROUP_W), bf16),
            pltpu.VMEM((seqs, groups * STATE, GROUP_W), bf16),
            pltpu.VMEM((seqs, groups * STATE, GROUP_W), bf16),
            pltpu.VMEM((rows, inner_dev), bf16),
            pltpu.VMEM((tp, seqs * own_len, inner_dev), bf16),
            pltpu.VMEM((seqs, groups * STATE, GROUP_W), bf16),
            *gather_sems(sp), *gather_sems(sp), *gather_sems(tp), *gather_sems(sp),
            dma((sp, tp, 1 + inner_factor(tp))), dma((sp, tp)),
            dma((2, seqs)),
            dma((seqs, gin)), dma((gin, seqs)),
            dma((seqs, groups)), dma((seqs, groups)),
            dma((seqs, tp)), dma((tp, seqs)),
        ],
        compiler_params=pltpu.CompilerParams(
            collective_id=0, has_side_effects=True, vmem_limit_bytes=56 * 2**20
        ),
    )(
        tokens, norm_gain[None, :], x_weight, z_weight, b_weight, c_weight, dt_weight.T,
        x_conv, b_conv, c_conv, dt_bias[None, :], decay_rate[None, :], out_gain[None, :], out_weight,
    )


def solution(mesh):
    return jax.shard_map(
        functools.partial(on_device, mesh.shape["sp"], mesh.shape["tp"]),
        mesh=mesh,
        in_specs=(
            P(None, ("sp", "tp"), None),
            P(),
            P("sp", "tp"),
            P("sp", "tp"),
            P("sp", "tp"),
            P("sp", "tp"),
            P("sp", "tp"),
            P(None, "tp"),
            P(None, "tp"),
            P(None, "tp"),
            P("tp"),
            P("tp"),
            P("tp"),
            P("tp", "sp"),
        ),
        out_specs=P(None, ("sp", "tp"), None),
        check_vma=False,
    )
```

```python
import functools

import jax
import jax.numpy as jnp
from jax import lax
from jax.experimental import pallas as pl
from jax.experimental.pallas import tpu as pltpu
from jax.sharding import PartitionSpec as P

HEADS = 16
HEAD_P = 64
STATE = 128
GROUPS = 8
CONV = 4
PER_GROUP = HEADS // GROUPS
GROUP_W = PER_GROUP * HEAD_P
LANES = 128
TILE = 16
epsilon = 1e-05
MESH = pl.DeviceIdType.MESH
f32 = jnp.float32
bf16 = jnp.bfloat16


def inner_factor(n):
    best = 1
    for d in range(1, n + 1):
        if n % d == 0 and d * d <= n:
            best = d
    return best


def silu(v):
    return v / (1.0 + jnp.exp(-v))


def expand(cols, group):
    first = group * PER_GROUP
    rows = cols.shape[0]
    lane = lax.broadcasted_iota(jnp.int32, (rows, GROUP_W), 1)
    wide = jnp.broadcast_to(cols[:, first : first + 1], (rows, GROUP_W))
    for k in range(1, PER_GROUP):
        wide = jnp.where(lane >= k * HEAD_P, cols[:, first + k : first + k + 1], wide)
    return wide


class Gather:
    def __init__(self, axis, n, own, slot, send, recv):
        self.axis, self.n, self.own, self.slot = axis, n, own, slot
        self.send, self.recv = send, recv
        self.inner = inner_factor(n)
        self.line = n // self.inner
        me = lax.axis_index(axis)
        self.me, self.a, self.b = me, me // self.inner, me % self.inner

    def target(self, index):
        if self.axis == "sp":
            return (index, lax.axis_index("tp"))
        return (lax.axis_index("sp"), index)

    def copy(self, j, way, index, own=False):
        return pltpu.make_async_remote_copy(
            src_ref=self.own if own else self.slot(j),
            dst_ref=self.slot(j),
            send_sem=self.send.at[j, way],
            recv_sem=self.recv.at[j],
            device_id=self.target(index),
            device_id_type=MESH,
        )

    def sends(self, j, right, left, do, own, peers=True):
        if right is not None:

            @pl.when(right)
            def _():
                do(self.copy(j, 0, self.me + self.inner, own))

        if left is not None:

            @pl.when(left)
            def _():
                do(self.copy(j, 1, self.me - self.inner, own))

        if peers:
            self.to_peers(j, do, own)

    def to_peers(self, j, do, own):
        for k in range(1, self.inner):
            do(self.copy(j, 1 + k, self.a * self.inner + (self.b + k) % self.inner, own))

    def start(self, peers=True):
        self.sends(self.me, self.a + 1 < self.line, self.a >= 1, lambda c: c.start(), True, peers)

    def pass_on(self):
        self.to_peers(self.me, lambda c: c.start(), True)
        for d in range(1, self.line):
            j = (self.a + d) % self.line * self.inner + self.b
            self.to_peers(j, lambda c: c.start(), False)

    def each(self, d, do, wait, peers=True):
        @pl.when(self.a >= d)
        def _():
            j = self.me - d * self.inner
            if wait:
                self.copy(j, 0, j).wait_recv()
            self.sends(j, self.a + 1 < self.line, None, do, False, peers)

        @pl.when(self.a + d < self.line)
        def _():
            j = self.me + d * self.inner
            if wait:
                self.copy(j, 0, j).wait_recv()
            self.sends(j, None, self.a >= 1, do, False, peers)

    def relay(self, d, peers=True):
        self.each(d, lambda c: c.start(), True, peers)

    def finish(self):
        for k in range(1, self.inner):
            b = (self.b + k) % self.inner
            for a in range(self.line):
                j = a * self.inner + b
                self.copy(j, 0, j).wait_recv()

    def drain(self):
        self.sends(self.me, self.a + 1 < self.line, self.a >= 1, lambda c: c.wait_send(), True)
        for d in range(1, self.line):
            self.each(d, lambda c: c.wait_send(), False)


def kernel(
    sp, tp, seqs, own_len, inner_dev, state_dev,
    tokens_in, norm_gain_in, x_weight, z_weight, b_weight, c_weight, dt_weight,
    x_conv, b_conv, c_conv, dt_bias_in, decay_rate_in, out_gain_in, out_weight_in,
    out,
    tokens, norm_gain, taps, dt_w, dt_bias, decay_rate, out_gain, out_weight, in_sem,
    wbuf, dtb, dtall, nbuf, wo, proj, halo, ext, bcb, xdt, cums, crow, ybuf, states, pin, pout, gated, gbuf, full,
    w_send, w_recv, d_send, d_recv, n_send, n_recv, o_send, o_recv, q_send, q_recv,
    h_sem, s_send, s_recv, c_send, c_recv, g_send, g_recv,
):
    spi, tpi = lax.axis_index("sp"), lax.axis_index("tp")
    d_model = tokens.shape[2]
    span = own_len * tp
    groups = state_dev // STATE
    conv_w = inner_dev + 2 * state_dev
    krows = x_weight.shape[0]
    heads_dev = dt_weight.shape[0]
    own_rows = seqs * own_len
    length = span * sp

    def rows_of(ref, j, size):
        return ref.at[pl.ds(pl.multiple_of(j * size, size), size), :]

    own_at = pl.ds(pl.multiple_of(spi * krows, krows), krows)
    moves = [(dt_weight, dt_w)]
    at = 0
    places = []
    for ref in (x_weight, b_weight, c_weight, z_weight):
        moves.append((ref, wbuf.at[own_at, pl.ds(at, ref.shape[1])]))
        places.append((at, ref.shape[1]))
        at += ref.shape[1]
    early = len(moves)
    moves += [(tokens_in, tokens), (norm_gain_in, norm_gain), (out_weight_in, out_weight)]
    middle = len(moves)
    at = 0
    for ref in (x_conv, b_conv, c_conv):
        moves.append((ref, taps.at[:, pl.ds(at, ref.shape[1])]))
        at += ref.shape[1]
    moves += [(dt_bias_in, dt_bias), (decay_rate_in, decay_rate), (out_gain_in, out_gain)]
    loads = [pltpu.make_async_copy(a, b, in_sem.at[k]) for k, (a, b) in enumerate(moves)]
    for load in loads:
        load.start()

    barrier = pltpu.get_barrier_semaphore()
    for k in range(1, sp):
        pl.semaphore_signal(barrier, inc=1, device_id=((spi + k) % sp, tpi), device_id_type=MESH)
    for k in range(1, tp):
        pl.semaphore_signal(barrier, inc=1, device_id=(spi, (tpi + k) % tp), device_id_type=MESH)
    for load in loads[:early]:
        load.wait()
    main_w = inner_dev * 2 + state_dev * 2
    pl.semaphore_wait(barrier, sp - 1 + tp - 1)

    def weight_gather(k):
        lo, width = places[k]

        def slot(j):
            return wbuf.at[pl.ds(pl.multiple_of(j * krows, krows), krows), pl.ds(lo, width)]

        return Gather("sp", sp, slot(spi), slot, w_send.at[k], w_recv.at[k])

    wg, zg = [weight_gather(k) for k in range(3)], weight_gather(3)
    dg = Gather("sp", sp, dt_w, lambda j: dtb.at[j], d_send, d_recv)
    dg.start()
    for g in wg:
        g.start()
    dtb[spi] = dt_w[...]
    for load in loads[early:middle]:
        load.wait()

    def norm_one(s, carry):
        src = tokens[s].astype(f32)
        scale = lax.rsqrt(jnp.mean(src * src, axis=-1, keepdims=True) + epsilon)
        at = pl.multiple_of(tpi * own_rows + s * own_len, own_len)
        nbuf[pl.ds(at, own_len), :] = (src * scale * norm_gain[...]).astype(bf16)
        return carry

    lax.fori_loop(0, seqs, norm_one, 0)
    ng = Gather("tp", tp, rows_of(nbuf, tpi, own_rows), lambda j: rows_of(nbuf, j, own_rows), n_send, n_recv)
    ng.start()
    wo[tpi, spi] = out_weight[...]
    og = Gather("sp", sp, out_weight, lambda j: wo.at[tpi, j], o_send, o_recv)

    def qg(j):
        return Gather("tp", tp, wo.at[tpi, j], lambda i: wo.at[i, j], q_send.at[j], q_recv.at[j])

    def q_each(own_peer, do):
        gin = og.inner

        def one(t, carry):
            if own_peer:
                do(qg(t * gin + og.b))
            else:
                for k in range(1, gin):
                    do(qg(t * gin + (og.b + k) % gin))
            return carry

        lax.fori_loop(0, og.line, one, 0)

    def q_relay(q):
        for d in range(1, q.line):
            q.relay(d)

    for d in range(1, max(og.line, ng.line)):
        if d < og.line:
            dg.relay(d)
            for g in wg:
                g.relay(d)
            for g in (og, zg):
                g.start() if d == 1 else g.relay(d - 1)
        if d < ng.line:
            ng.relay(d)
    if og.line == 1:
        og.start()
        zg.start()
    for load in loads[middle:]:
        load.wait()
    ng.finish()
    for g in wg:
        g.finish()
    dg.finish()

    step_n = 2 * LANES
    for j in range(sp):
        dtall[:heads_dev, j * krows : (j + 1) * krows] = dtb[j]

    def project(i, carry):
        block = nbuf[pl.ds(pl.multiple_of(i * own_rows, own_rows), own_rows), :]
        for lo in range(0, conv_w, step_n):
            hi = min(conv_w, lo + step_n)
            res = jnp.dot(block, wbuf[:, lo:hi], preferred_element_type=f32).astype(bf16)
            for s in range(seqs):
                at = pl.multiple_of(s * span + i * own_len, own_len)
                proj[pl.ds(at, own_len), lo:hi] = res[s * own_len : (s + 1) * own_len]
        res = lax.dot_general(
            block, dtall[...], (((1,), (1,)), ((), ())), preferred_element_type=f32
        ).astype(bf16)
        for s in range(seqs):
            at = pl.multiple_of(s * span + i * own_len, own_len)
            proj[pl.ds(at, own_len), main_w : main_w + heads_dev] = res[s * own_len : (s + 1) * own_len, :heads_dev]
        return carry

    lax.fori_loop(0, tp, project, 0)

    def project_z(i):
        block = nbuf[pl.ds(pl.multiple_of(i * own_rows, own_rows), own_rows), :]
        res = jnp.dot(block, wbuf[:, conv_w:main_w], preferred_element_type=f32).astype(bf16)
        for s in range(seqs):
            at = pl.multiple_of(s * span + i * own_len, own_len)
            proj[pl.ds(at, own_len), conv_w:main_w] = res[s * own_len : (s + 1) * own_len]

    def halo_copy(s):
        return pltpu.make_async_remote_copy(
            src_ref=proj.at[pl.ds(s * span + span - TILE, TILE), pl.ds(0, conv_w)],
            dst_ref=halo.at[s],
            send_sem=h_sem.at[0, s],
            recv_sem=h_sem.at[1, s],
            device_id=(lax.rem(spi + 1, sp), tpi),
            device_id_type=MESH,
        )

    @pl.when(spi + 1 < sp)
    def _():
        for s in range(seqs):
            halo_copy(s).start()

    if og.line > 1:
        og.relay(og.line - 1)
        zg.relay(og.line - 1)
    row_i = lax.broadcasted_iota(jnp.int32, (span, span), 0)
    col_i = lax.broadcasted_iota(jnp.int32, (span, span), 1)
    lower = (row_i >= col_i).astype(f32)
    upper = (row_i <= col_i).astype(f32)

    def decay_of(s, carry):
        at = pl.ds(pl.multiple_of(s * span, span), span)
        raw = proj[at, conv_w + inner_dev : conv_w + inner_dev + heads_dev].astype(f32) + dt_bias[...]
        dt = jnp.maximum(raw, 0.0) + jnp.log1p(jnp.exp(-jnp.abs(raw)))
        log = -(dt * decay_rate[...]) / length
        cums[at, :heads_dev] = dt
        cums[at, LANES : LANES + heads_dev] = jnp.dot(lower, log, preferred_element_type=f32, precision=lax.Precision.HIGHEST)
        across = lax.dot_general(
            log, upper, (((0,), (0,)), ((), ())),
            preferred_element_type=f32, precision=lax.Precision.HIGHEST,
        )
        crow[s, :heads_dev] = across
        return carry

    lax.fori_loop(0, seqs, decay_of, 0)

    @pl.when(spi >= 1)
    def _():
        for s in range(seqs):
            halo_copy(s).wait_recv()

    @pl.when(spi == 0)
    def _():
        halo[...] = jnp.zeros_like(halo)

    gin = inner_factor(sp)
    line = sp // gin
    za, zb = spi // gin, spi % gin

    def peer_copy(s, b, k):
        return pltpu.make_async_remote_copy(
            src_ref=states.at[b, s],
            dst_ref=states.at[b, s],
            send_sem=s_send.at[s, k],
            recv_sem=s_recv.at[b, s],
            device_id=(za * gin + (zb + k) % gin, tpi),
            device_id_type=MESH,
        )

    def local(s):
        at = pl.ds(pl.multiple_of(s * span, span), span)
        for lo in range(0, conv_w, LANES):
            part = slice(lo, lo + LANES)
            ext[0:TILE, part] = halo[s, :, part].astype(f32)
            ext[TILE:, part] = proj[at, part].astype(f32)
        dt = cums[at, :LANES]
        cum = cums[at, LANES:]

        def conv(lo):
            part = slice(lo, lo + LANES)
            total = taps[0:1, part] * ext[TILE - CONV + 1 : TILE - CONV + 1 + span, part]
            for k in range(1, CONV):
                begin = TILE - CONV + 1 + k
                total = total + taps[k : k + 1, part] * ext[begin : begin + span, part]
            return silu(total)

        for g in range(groups):
            xd = conv(g * GROUP_W) * expand(dt, g)
            bg = conv(inner_dev + g * STATE).astype(bf16)
            cg = conv(inner_dev + state_dev + g * STATE).astype(bf16)
            wide = expand(cum, g)
            last = wide[span - 1 : span, :]
            xdt[at, g * GROUP_W : (g + 1) * GROUP_W] = xd.astype(bf16)
            bcb[at, g * STATE : (g + 1) * STATE] = bg
            bcb[at, state_dev + g * STATE : state_dev + (g + 1) * STATE] = cg
            st = lax.dot_general(
                bg, (xd * jnp.exp(last - wide)).astype(bf16), (((0,), (0,)), ((), ())),
                preferred_element_type=f32,
            )
            states[zb, s, g * STATE : (g + 1) * STATE, :] = st.astype(bf16)
            fade_at = groups * STATE + g * TILE
            states[zb, s, fade_at : fade_at + TILE, :] = (
                jnp.broadcast_to(jnp.exp(last), (TILE, GROUP_W)).astype(bf16)
            )
        for k in range(1, gin):
            peer_copy(s, zb, k).start()

    def chain_copy(s, g):
        part = pl.ds(g * STATE, STATE)
        return pltpu.make_async_remote_copy(
            src_ref=pout.at[s, part, :],
            dst_ref=pin.at[s, part, :],
            send_sem=c_send.at[s, g],
            recv_sem=c_recv.at[s, g],
            device_id=(lax.rem(spi + gin, sp), tpi),
            device_id_type=MESH,
        )

    def chain(s):
        for k in range(1, gin):
            peer_copy(s, (zb + k) % gin, k).wait_recv()

        @pl.when(za == 0)
        def _():
            pin[s] = jnp.zeros(pin.shape[1:], bf16)

        for g in range(groups):
            part = slice(g * STATE, (g + 1) * STATE)

            @pl.when(za >= 1)
            def _():
                chain_copy(s, g).wait_recv()

            total = pin[s, part, :].astype(f32)
            mine = total
            for b in range(gin):
                mine = jnp.where(zb == b, total, mine)
                fade = states[b, s, groups * STATE + g * TILE : groups * STATE + (g + 1) * TILE, :].astype(f32)
                total = total * fade[0:1, :] + states[b, s, part, :].astype(f32)
            pout[s, part, :] = total.astype(bf16)

            @pl.when(za + 1 < line)
            def _():
                chain_copy(s, g).start()

            full[s, part, :] = mine.astype(bf16)

    def diagonal(s):
        at = pl.ds(pl.multiple_of(s * span, span), span)
        cum = cums[at, LANES:]
        lane = lax.broadcasted_iota(jnp.int32, (span, GROUP_W), 1)
        mask = lax.broadcasted_iota(jnp.int32, (span, span), 0) >= lax.broadcasted_iota(jnp.int32, (span, span), 1)
        for g in range(groups):
            bg = bcb[at, g * STATE : (g + 1) * STATE]
            cg = bcb[at, state_dev + g * STATE : state_dev + (g + 1) * STATE]
            xg = xdt[at, g * GROUP_W : (g + 1) * GROUP_W]
            scores = lax.dot_general(cg, bg, (((1,), (1,)), ((), ())), preferred_element_type=f32)
            yg = None
            for k in range(PER_GROUP):
                h = g * PER_GROUP + k
                gaps = jnp.where(mask, cum[:, h : h + 1] - crow[s, h : h + 1, :], -jnp.inf)
                part = jnp.dot((scores * jnp.exp(gaps)).astype(bf16), xg, preferred_element_type=f32)
                yg = part if yg is None else jnp.where(lane >= k * HEAD_P, part, yg)
            ybuf[at, g * GROUP_W : (g + 1) * GROUP_W] = yg

    lag, hop = 2, 2
    first = lag + hop * za

    def steps(t, carry):
        @pl.when(t < seqs)
        def _():
            local(t)

        @pl.when((t >= first) & (t - first < seqs))
        def _():
            chain(t - first)

        @pl.when((t >= seqs) & (t < 2 * seqs))
        def _():
            diagonal(t - seqs)

        @pl.when(t == seqs)
        def _():
            og.finish()
            q_each(True, lambda q: q.start())
            q_each(False, lambda q: q.start())

        @pl.when(t == 2 * seqs)
        def _():
            zg.finish()

        @pl.when((t >= 2 * seqs) & (t < 2 * seqs + tp))
        def _():
            project_z(t - 2 * seqs)

        return carry

    lax.fori_loop(0, max(2 * seqs + tp, lag + hop * (line - 1) + seqs), steps, 0)
    q_each(True, q_relay)
    q_each(False, q_relay)

    def a2a_copy(s, k):
        to = (tpi + k) % tp
        return pltpu.make_async_remote_copy(
            src_ref=gated.at[pl.ds(pl.multiple_of(s * span + to * own_len, own_len), own_len), :],
            dst_ref=gbuf.at[tpi, pl.ds(pl.multiple_of(s * own_len, own_len), own_len), :],
            send_sem=g_send.at[s, k],
            recv_sem=g_recv.at[tpi, s],
            device_id=(spi, to),
            device_id_type=MESH,
        )

    def a2a_wait(s, k):
        frm = (tpi + k) % tp
        pltpu.make_async_remote_copy(
            src_ref=gated.at[pl.ds(0, own_len), :],
            dst_ref=gbuf.at[frm, pl.ds(pl.multiple_of(s * own_len, own_len), own_len), :],
            send_sem=g_send.at[s, k],
            recv_sem=g_recv.at[frm, s],
            device_id=(spi, frm),
            device_id_type=MESH,
        ).wait_recv()

    def finish(s, carry):
        at = pl.ds(pl.multiple_of(s * span, span), span)
        cum = cums[at, LANES:]
        for g in range(groups):
            part = slice(g * GROUP_W, (g + 1) * GROUP_W)
            cg = bcb[at, state_dev + g * STATE : state_dev + (g + 1) * STATE]
            carried = jnp.dot(cg, full[s, g * STATE : (g + 1) * STATE, :], preferred_element_type=f32)
            y = ybuf[at, part] + carried * jnp.exp(expand(cum, g))
            z = proj[at, conv_w + g * GROUP_W : conv_w + (g + 1) * GROUP_W].astype(f32)
            v = y * silu(z)
            v = v * lax.rsqrt(jnp.mean(v * v, axis=-1, keepdims=True) + epsilon)
            gated[at, part] = (v * out_gain[:, part]).astype(bf16)
        for k in range(1, tp):
            a2a_copy(s, k).start()
        own_at = pl.multiple_of(s * span + tpi * own_len, own_len)
        gbuf[tpi, pl.ds(pl.multiple_of(s * own_len, own_len), own_len), :] = gated[pl.ds(own_at, own_len), :]
        return carry

    lax.fori_loop(0, seqs, finish, 0)
    q_each(True, lambda q: q.finish())
    q_each(False, lambda q: q.finish())
    for s in range(seqs):
        for k in range(1, tp):
            a2a_wait(s, k)

    width = out_weight.shape[1]
    for j in range(sp):
        total = jnp.dot(gbuf[0], wo[0, j], preferred_element_type=f32)
        for i in range(1, tp):
            total = total + jnp.dot(gbuf[i], wo[i, j], preferred_element_type=f32)
        res = total.astype(bf16)
        for s in range(seqs):
            out[s, :, j * width : (j + 1) * width] = res[s * own_len : (s + 1) * own_len]

    for gather in (*wg, zg, dg, ng, og):
        gather.drain()
    q_each(True, lambda q: q.drain())
    q_each(False, lambda q: q.drain())
    for s in range(seqs):
        for k in range(1, gin):
            peer_copy(s, zb, k).wait_send()
        for k in range(1, tp):
            a2a_copy(s, k).wait_send()

    @pl.when(spi + 1 < sp)
    def _():
        for s in range(seqs):
            halo_copy(s).wait_send()

    @pl.when(za + 1 < line)
    def _():
        for s in range(seqs):
            for g in range(groups):
                chain_copy(s, g).wait_send()


def on_device(
    sp, tp, tokens, norm_gain, x_weight, z_weight, b_weight, c_weight, dt_weight,
    x_conv, b_conv, c_conv, dt_bias, decay_rate, out_gain, out_weight,
):
    seqs, own_len, d_model = tokens.shape
    inner_dev, state_dev = x_weight.shape[1], b_weight.shape[1]
    groups = state_dev // STATE
    span = own_len * tp
    rows = seqs * span
    cols = 2 * inner_dev + 2 * state_dev
    conv_w = inner_dev + 2 * state_dev
    gin = inner_factor(sp)
    vmem = pl.BlockSpec(memory_space=pltpu.VMEM)
    dma = pltpu.SemaphoreType.DMA

    def gather_sems(n):
        return [dma((n, 1 + max(inner_factor(n), 1))), dma((n,))]

    return pl.pallas_call(
        functools.partial(kernel, sp, tp, seqs, own_len, inner_dev, state_dev),
        out_shape=jax.ShapeDtypeStruct(tokens.shape, bf16),
        in_specs=[pl.BlockSpec(memory_space=pl.ANY)] * 14,
        out_specs=vmem,
        scratch_shapes=[
            pltpu.VMEM(tokens.shape, bf16),
            pltpu.VMEM((1, d_model), f32),
            pltpu.VMEM((x_conv.shape[0], conv_w), f32),
            pltpu.VMEM(dt_weight.shape[::-1], bf16),
            pltpu.VMEM((1, dt_weight.shape[1]), f32),
            pltpu.VMEM((1, dt_weight.shape[1]), f32),
            pltpu.VMEM((1, inner_dev), f32),
            pltpu.VMEM(out_weight.shape, bf16),
            dma((14,)),
            pltpu.VMEM((d_model, cols), bf16),
            pltpu.VMEM((sp,) + dt_weight.shape[::-1], bf16),
            pltpu.VMEM((TILE, d_model), bf16),
            pltpu.VMEM((rows, d_model), bf16),
            pltpu.VMEM((tp, sp) + out_weight.shape, bf16),
            pltpu.VMEM((rows, cols + LANES), bf16),
            pltpu.VMEM((seqs, TILE, conv_w), bf16),
            pltpu.VMEM((TILE + span, conv_w), f32),
            pltpu.VMEM((rows, 2 * state_dev), bf16),
            pltpu.VMEM((rows, inner_dev), bf16),
            pltpu.VMEM((rows, 2 * LANES), f32),
            pltpu.VMEM((seqs, 8, span), f32),
            pltpu.VMEM((rows, inner_dev), f32),
            pltpu.VMEM((gin, seqs, groups * (STATE + TILE), GROUP_W), bf16),
            pltpu.VMEM((seqs, groups * STATE, GROUP_W), bf16),
            pltpu.VMEM((seqs, groups * STATE, GROUP_W), bf16),
            pltpu.VMEM((rows, inner_dev), bf16),
            pltpu.VMEM((tp, seqs * own_len, inner_dev), bf16),
            pltpu.VMEM((seqs, groups * STATE, GROUP_W), bf16),
            dma((4, sp, 1 + gin)), dma((4, sp)),
            *gather_sems(sp), *gather_sems(tp), *gather_sems(sp),
            dma((sp, tp, 1 + inner_factor(tp))), dma((sp, tp)),
            dma((2, seqs)),
            dma((seqs, gin)), dma((gin, seqs)),
            dma((seqs, groups)), dma((seqs, groups)),
            dma((seqs, tp)), dma((tp, seqs)),
        ],
        compiler_params=pltpu.CompilerParams(
            collective_id=0, has_side_effects=True, vmem_limit_bytes=56 * 2**20
        ),
    )(
        tokens, norm_gain[None, :], x_weight, z_weight, b_weight, c_weight, dt_weight.T,
        x_conv, b_conv, c_conv, dt_bias[None, :], decay_rate[None, :], out_gain[None, :], out_weight,
    )


def solution(mesh):
    return jax.shard_map(
        functools.partial(on_device, mesh.shape["sp"], mesh.shape["tp"]),
        mesh=mesh,
        in_specs=(
            P(None, ("sp", "tp"), None),
            P(),
            P("sp", "tp"),
            P("sp", "tp"),
            P("sp", "tp"),
            P("sp", "tp"),
            P("sp", "tp"),
            P(None, "tp"),
            P(None, "tp"),
            P(None, "tp"),
            P("tp"),
            P("tp"),
            P("tp"),
            P("tp", "sp"),
        ),
        out_specs=P(None, ("sp", "tp"), None),
        check_vma=False,
    )
```
